32 devices in a mesh: ep: 8 (over z, x), tp: 4 (over y, core).
Axes of the slice: x: 2, y: 2, z: 4, core: 2. Of those that a mesh axis runs over, the one named last changes fastest.
Arguments:
- mix_query: bfloat16 [2048, 2048], P('ep', 'tp'), may hold values from -6 to 6
- forget_input: bfloat16 [2048, 2048], P('ep', 'tp'), may hold values from -6 to 6
- mix_value: bfloat16 [2048, 2048], P('ep', 'tp'), may hold values from -6 to 6
- out_gate_input: bfloat16 [2048, 2048], P('ep', 'tp'), may hold values from -6 to 6
- decay_shift: float32 [2048, 16], P('ep', 'tp'), may hold values from -1.5 to 0
- forget_floor: float32 [2048], P('tp'), may hold values from 0.9 to 1
- head_gain: float32 [128], replicated, may hold values from 0.1 to 1.9
- w_mix_out: bfloat16 [2048, 2048], P(None, 'tp'), may hold values from -0.125 to 0.125
- moe_input: bfloat16 [2048, 2048], P('ep'), may hold values from -6 to 6
- moe_gain: float32 [2048], replicated, may hold values from 0.1 to 1.9
- routes: int32 [2048, 2], P('ep'), may hold values from 0 to 7, all different within a row; in each aligned block of 256 rows (0 to 255, 256 to 511, ...) at most 80 rows name the same one
- route_weight: float32 [2048, 2], P('ep'), may hold values from 0.1 to 1
- w_exp_gate: bfloat16 [8, 2048, 4096], P('ep', None, 'tp'), may hold values from -0.125 to 0.125
- w_exp_up: bfloat16 [8, 2048, 4096], P('ep', None, 'tp'), may hold values from -0.125 to 0.125
- w_exp_down: bfloat16 [8, 4096, 2048], P('ep', 'tp'), may hold values from -0.125 to 0.125
Outputs:
- mixed: bfloat16 [2048, 2048], P('ep', 'tp')
- moe_out: bfloat16 [2048, 2048], P('ep', 'tp')
The draws below stay inside these ranges and needn't reach their ends.
Inputs may be any that keep to these rules, and one draw needn't show every extreme that they name: `routes`: at most 80 of the rows of one index of ep name one expert, and in every draw some device's rows name one expert exactly 80 times; the experts of a row differ.
All inputs are finite; a program needn't handle non-finite values.
Results may differ from the reference program's by a relative error of at most 0.02.
Values may be sent and summed in bfloat16 or wider, within the bound.
A program may use at most 64 MiB of HBM per device.

```python
import math
import jax
import jax.numpy as jnp
import numpy as np
from jax import lax

D = 2048
HEADS = 16
DK = 128
FE = 4096
TOP_K = 2
BLOCK = 64
TOK_DEV = 256
HW = 2048
TOKENS = 2048
EXPERTS = 8
CAP = 80
N_EP = 8
N_TP = 4


def draw_forget_floor(key, part):
    length = TOK_DEV * N_EP
    subkeys = jax.random.split(key, 3)
    fast_share = 0.5
    fast_heads = jax.random.bernoulli(subkeys[0], fast_share, (HEADS,))
    fast_rate = jnp.exp(jax.random.uniform(subkeys[1], (HEADS, DK), jnp.float32, math.log(0.02), math.log(0.07)))
    slow_rate = jnp.exp(jax.random.uniform(subkeys[2], (HEADS, DK), jnp.float32, math.log(0.3), 0.0)) / length
    keep_rate = jnp.where(fast_heads[:, None], fast_rate, slow_rate)
    return (1.0 - keep_rate).reshape(HEADS * DK).astype(jnp.float32)


def draw_decay_shift(key, part):
    length = TOK_DEV * N_EP
    subkeys = jax.random.split(key, 3)
    factor = jnp.exp(jax.random.uniform(subkeys[0], (N_EP, HEADS), jnp.float32, -math.log(2.0), math.log(2.0)))
    steady = -0.4 * jnp.repeat(factor, TOK_DEV, axis=0) / length
    places = jax.random.randint(subkeys[1], (2, HEADS), 0, length)
    depths = jnp.log(jax.random.uniform(subkeys[2], (2, HEADS), jnp.float32, 0.55, 0.8))
    marked = (jnp.arange(length)[:, None, None] == places[None, :, :]).astype(jnp.float32)
    return (steady + jnp.sum(marked * depths[None, :, :], axis=1)).astype(jnp.float32)


def spiked(result, stream_key, source, target, blocks, factor):
    owner, partner = [(jnp.arange(result.shape[axis_at]) // (result.shape[axis_at] // blocks)).reshape([-1 if axis == axis_at else 1 for axis in range(result.ndim)]) for axis_at in (source, target)]
    chosen = jax.random.permutation(stream_key, blocks)[partner]
    strong = (owner == chosen) | (owner == (partner + blocks // 2) % blocks)
    return jnp.where(strong, factor * result, result)


def block_levels(own_key, extent, pieces, smallest, largest):
    loudness = 1.0
    for dim, shards_of in pieces:
        draws = jax.random.uniform(jax.random.fold_in(jax.random.fold_in(own_key, 6), dim), (shards_of,), jnp.float32, smallest / len(pieces), largest / len(pieces))
        loudness = loudness * jnp.repeat(jnp.exp(draws), extent[dim] // shards_of).reshape((-1,) + (1,) * (len(extent) - 1 - dim))
    return loudness


def assign_block(stream_key, own, number, rows, amount, top, reach, slope):
    sequence = jax.random.permutation(stream_key, amount)
    heavy_load, common = shares(amount, rows * top, reach, slope, True), shares(amount, rows * top, reach, slope, False)
    places = jnp.arange(amount)

    def named(tallies, offset_by):
        used = int((tallies > 0).sum())
        fixed = max(1, used // 4)
        moved = fixed + (places - fixed + offset_by * (used - fixed)) % max(1, amount - fixed)
        return jnp.zeros((amount,), jnp.int32).at[sequence[jnp.where(places < fixed, places, moved)]].set(jnp.asarray(tallies, jnp.int32))

    tallies = jnp.where(number % 4 == 0, named(heavy_load, number // 4), named(common, number - number // 4 - 1))
    mixed = jax.random.permutation(jax.random.fold_in(own, 3), amount)
    donor, taker = mixed[0:amount // 2 * 2:2], mixed[1:amount // 2 * 2:2]
    margin = jnp.minimum(tallies[donor] - 1, reach - tallies[taker]) // 2
    margin = jnp.where((donor == sequence[0]) | (taker == sequence[0]) | (tallies[taker] == 0), 0, jnp.maximum(margin, 0))
    moved = jax.random.randint(jax.random.fold_in(own, 4), (amount // 2,), 0, 1 << 20) % (margin + 1)
    tallies = tallies.at[donor].add(-moved).at[taker].add(moved)
    labels = jnp.searchsorted(jnp.cumsum(tallies), jnp.arange(rows * top), side="right").astype(jnp.int32)
    grid = labels.reshape(top, rows).T
    grid = grid[jax.random.permutation(jax.random.fold_in(own, 1), rows)]
    offset_by = jax.random.randint(jax.random.fold_in(own, 2), (rows, 1), 0, top)
    return jnp.take_along_axis(grid, (jnp.arange(top)[None, :] + offset_by) % top, axis=1)


def shares(number_of, total, bound, skew, full):
    portions = [(1 << 20) // math.isqrt(rank ** skew) + 1 for rank in range(1, number_of + 1)]
    largest = bound if full else min(bound, max(-(-total // number_of), total * portions[0] // sum(portions)))
    least = 1 if total - largest >= number_of - 1 else 0
    given, rest = [largest] + [least] * (number_of - 1), total - largest - least * (number_of - 1)
    while rest > 0:
        movable = [i for i in range(1, number_of) if given[i] < largest] or [i for i in range(1, number_of) if given[i] < bound]
        mass, remaining = sum([portions[i] for i in movable]), rest
        for i in movable:
            addition = min(bound - given[i], max(1, remaining * portions[i] // mass), rest)
            given[i] = given[i] + addition
            rest = rest - addition
    return np.array(given)


def centred(stream_key, extent, scale, bound, pieces=(), kind=jnp.bfloat16):
    drawn = scale * jax.random.normal(stream_key, extent, jnp.float32)
    if pieces:
        drawn = drawn * block_levels(stream_key, extent, pieces, -0.22, 0.18)
    return jnp.clip(drawn, -bound, bound).astype(kind)


def bell_draw_with(key, shape, scale, reach, cuts, heavy, held_as=jnp.bfloat16):
    values = scale * jax.random.normal(key, shape, jnp.float32)
    if cuts:
        values = values * block_levels(key, shape, cuts, -0.22, 0.18)
    return jnp.clip(spiked(values, jax.random.fold_in(key, 3), *heavy), -reach, reach).astype(held_as)


def setup_inputs(seed: int = 0) -> dict:
    key_of = jax.random.split(jax.random.key(seed), 16)
    mix_query = centred(key_of[0], (TOKENS, HW), 1.0, 6.0, ((0, 8), (1, 4)))
    forget_input = centred(key_of[1], (TOKENS, HW), 1.0, 6.0, ((0, 8), (1, 4)))
    mix_value = centred(key_of[2], (TOKENS, HW), 1.0, 6.0, ((0, 8), (1, 4)))
    out_gate_input = centred(key_of[3], (TOKENS, HW), 1.0, 6.0, ((0, 8), (1, 4)))
    decay_shift = draw_decay_shift(jax.random.fold_in(key_of[15], 71), 0)
    forget_floor = draw_forget_floor(jax.random.fold_in(key_of[15], 71), 0)
    head_gain = jnp.clip(1.0 + 0.18 * jax.random.normal(key_of[6], (DK,), jnp.float32), 0.1, 1.9)
    w_mix_out = centred(key_of[7], (HW, D), HW ** -0.5, 0.125, ((1, 4),))
    moe_input = centred(key_of[8], (TOKENS, D), 1.0, 6.0, ((0, 8),))
    moe_gain = jnp.clip(1.0 + 0.18 * jax.random.normal(key_of[9], (D,), jnp.float32), 0.1, 1.9)
    routes_keys = jax.random.split(jax.random.fold_in(key_of[10], 1), TOKENS // TOK_DEV)
    routes_turns = jax.random.permutation(jax.random.fold_in(key_of[10], 3), TOKENS // TOK_DEV)
    routes = jax.vmap(lambda own, number: assign_block(jax.random.fold_in(key_of[10], 2), own, number, TOK_DEV, EXPERTS, TOP_K, CAP, 1))(routes_keys, routes_turns).reshape((TOKENS, TOP_K))
    route_weight = jnp.clip(0.1 + 0.9 * jax.random.uniform(key_of[11], (TOKENS, TOP_K), jnp.float32) ** block_levels(key_of[11], (TOKENS, TOP_K), ((0, 8),), -0.2, 0.2), 0.1, 1.0)
    w_exp_gate = centred(key_of[12], (EXPERTS, D, FE), D ** -0.5, 0.125, ((0, 8), (2, 4)))
    w_exp_up = centred(key_of[13], (EXPERTS, D, FE), D ** -0.5, 0.125, ((0, 8), (2, 4)))
    w_exp_down = bell_draw_with(key_of[14], (EXPERTS, FE, D), FE ** -0.5, 0.125, ((0, 8), (1, 4)), (1, 2, 4, 2.0))
    return {"mix_query": mix_query, "forget_input": forget_input, "mix_value": mix_value, "out_gate_input": out_gate_input, "decay_shift": decay_shift, "forget_floor": forget_floor, "head_gain": head_gain, "w_mix_out": w_mix_out, "moe_input": moe_input, "moe_gain": moe_gain, "routes": routes, "route_weight": route_weight, "w_exp_gate": w_exp_gate, "w_exp_up": w_exp_up, "w_exp_down": w_exp_down}


eps = 1e-06
highest_precision = lax.Precision.HIGHEST

def recurrence(query, input_gate, values, log_decay):
    length = query.shape[0]
    blocks = length // BLOCK

    def to_blocks(array):
        return array.reshape(blocks, BLOCK, HEADS, DK).transpose(0, 2, 1, 3)
    causal = jnp.tril(jnp.ones((BLOCK, BLOCK), bool))[:, :, None]

    def advance(recurrent_state, inputs):
        query_block, key_block, value_block, g_block = inputs
        running_decay = jnp.cumsum(g_block, axis=1)
        spread = running_decay[:, :, None, :] - running_decay[:, None, :, :]
        weights = jnp.where(causal, jnp.exp(jnp.minimum(spread, 0.0)), 0.0)
        scores = jnp.einsum('htk,htsk,hsk->hts', query_block, weights, key_block, precision=highest_precision)
        block_result = jnp.einsum('hts,hsv->htv', scores, value_block, precision=highest_precision)
        block_result = block_result + jnp.einsum('rsd,rda->rsa', query_block * jnp.exp(running_decay), recurrent_state, precision=highest_precision)
        closing_total = running_decay[:, -1:, :]
        carried_over_state = jnp.einsum('gbx,gbi->gxi', key_block * jnp.exp(closing_total - running_decay), value_block, precision=highest_precision)
        recurrent_state = jnp.exp(closing_total[:, 0, :])[:, :, None] * recurrent_state + carried_over_state
        return (recurrent_state, block_result)
    initial = jnp.zeros((HEADS, DK, DK), jnp.float32)
    _, block_result = lax.scan(advance, initial, (to_blocks(query), to_blocks(input_gate), to_blocks(values), to_blocks(log_decay)))
    return block_result.transpose(0, 2, 1, 3).reshape(length, HEADS, DK)

def token_mixer(mix_query, forget_input, mix_value, out_gate_input, decay_shift, forget_floor, head_gain, w_mix_out):
    length = mix_query.shape[0]
    gate_input = forget_input.astype(jnp.float32)
    forget = forget_floor + (1.0 - forget_floor) * jax.nn.sigmoid(gate_input)
    input_gate = (1.0 - forget_floor) * jax.nn.sigmoid(-gate_input)
    log_decay = jnp.log(forget) + jnp.repeat(decay_shift, DK, axis=1)
    block_result = recurrence(mix_query.astype(jnp.float32), input_gate, mix_value.astype(jnp.float32), log_decay)
    inverse = lax.rsqrt(lax.optimization_barrier(jnp.mean(block_result * block_result, axis=2, keepdims=True)) + eps)
    gated = jax.nn.silu(out_gate_input.astype(jnp.float32)).reshape(length, HEADS, DK)
    head_out = (block_result * inverse * head_gain * gated).reshape(length, HEADS * DK).astype(jnp.bfloat16)
    return jnp.dot(head_out, w_mix_out, preferred_element_type=jnp.float32).astype(jnp.bfloat16)

def experts_layer(moe_input, moe_gain, routes, route_weight, w_exp_gate, w_exp_up, w_exp_down):
    token_rows = moe_input.astype(jnp.float32)
    inverse = lax.rsqrt(lax.optimization_barrier(jnp.mean(token_rows * token_rows, axis=1, keepdims=True)) + eps)
    normed = (token_rows * inverse * moe_gain).astype(jnp.bfloat16)
    flat_ids = routes.reshape(-1)
    pair_count = flat_ids.shape[0]
    slot_count = CAP * N_EP
    group_size = FE // N_TP

    def one_expert(expert):
        matches = flat_ids == expert
        chosen = jnp.nonzero(matches, size=slot_count, fill_value=0)[0].astype(jnp.int32)
        how_many = jnp.sum(matches.astype(jnp.int32))
        usable = jnp.arange(slot_count, dtype=jnp.int32) < how_many
        picked = normed[chosen // TOP_K]
        gate_sum = jnp.dot(picked, w_exp_gate[expert], preferred_element_type=jnp.float32)
        up_sum = jnp.dot(picked, w_exp_up[expert], preferred_element_type=jnp.float32)
        hidden = (jax.nn.silu(gate_sum) * up_sum).astype(jnp.bfloat16)
        grouped = hidden.reshape(slot_count, N_TP, group_size).astype(jnp.float32)
        down_groups = w_exp_down[expert].reshape(N_TP, group_size, D).astype(jnp.float32)
        partial_value = jnp.einsum('sgf,gfd->sgd', grouped, down_groups).astype(jnp.bfloat16)
        summed = lax.optimization_barrier(jnp.sum(partial_value.astype(jnp.float32), axis=1)).astype(jnp.bfloat16)
        return (chosen, jnp.where(usable[:, None], summed, jnp.zeros_like(summed)))
    chosen_all, outputs = lax.map(one_expert, jnp.arange(EXPERTS, dtype=jnp.int32))
    pair_out = jnp.zeros((pair_count, D), jnp.float32).at[chosen_all.reshape(-1)].add(outputs.reshape(-1, D).astype(jnp.float32))
    combined = lax.optimization_barrier(jnp.sum(pair_out.reshape(-1, TOP_K, D) * route_weight[:, :, None], axis=1))
    return combined.astype(jnp.bfloat16)

def reference(mix_query, forget_input, mix_value, out_gate_input, decay_shift, forget_floor, head_gain, w_mix_out, moe_input, moe_gain, routes, route_weight, w_exp_gate, w_exp_up, w_exp_down):
    mixed = token_mixer(mix_query, forget_input, mix_value, out_gate_input, decay_shift, forget_floor, head_gain, w_mix_out)
    moe_out = experts_layer(moe_input, moe_gain, routes, route_weight, w_exp_gate, w_exp_up, w_exp_down)
    return (mixed, moe_out)
```

```python
import functools

import jax
import jax.numpy as jnp
from jax import lax
from jax.experimental import pallas as pl
from jax.experimental.pallas import tpu as pltpu
from jax.sharding import PartitionSpec as P

TOP_K = 2
EPS = 1e-06
MESH = pl.DeviceIdType.MESH
BF = jnp.bfloat16
F32 = jnp.float32
HIGH = lax.Precision.HIGHEST


def mm(a, b, dims=((1,), (0,)), precision=None):
    return lax.dot_general(
        a, b, (dims, ((), ())), preferred_element_type=F32, precision=precision
    )


def scan_windows(ep):
    windows = [0]
    w = 1
    while w < ep - 1:
        windows.append(w)
        w *= 2
    return windows


def kernel(
    cfg,
    q_ref,
    fi_ref,
    v_ref,
    og_ref,
    ds_ref,
    ff_ref,
    hg_ref,
    x_ref,
    mg_ref,
    rt_ref,
    rw_ref,
    wm_hbm,
    wg_hbm,
    wu_hbm,
    wd_hbm,
    mixed_ref,
    moe_ref,
    wm,
    wg,
    wu,
    wd,
    disp,
    xs,
    hid,
    snd_p,
    rs_p,
    own,
    snd_y,
    rs_y,
    fin,
    ret,
    pick,
    ks_s,
    ks_r,
    carry,
    intra,
    qdec,
    ho,
    w_sem,
    a_ss,
    a_rs,
    gy_ss,
    gy_rs,
    gp_ss,
    gp_rs,
    rp_ss,
    rp_rs,
    ry_ss,
    ry_rs,
    b_ss,
    b_rs,
    k_ss,
    k_rs,
    hy_ss,
    hy_rs,
    hp_ss,
    hp_rs,
):
    ep, tp, cap, groups = cfg
    gb = ep // groups
    ny = tp // 2
    me = lax.axis_index("ep")
    t = lax.axis_index("tp")
    y = t // 2
    c = t % 2
    mate = y * 2 + (1 - c)
    rows, dim = x_ref.shape
    width = dim // tp
    slots = ep * cap
    hidden_units = wg.shape[1]
    heads = ds_ref.shape[1]
    hs = hg_ref.shape[1]
    hw = q_ref.shape[1]

    def ring(a, n):
        return lax.rem(a + n, n)

    def up_y(dy):
        return ring(y + dy, ny)

    def dn_y(dy):
        return ring(y - dy, ny)

    def rc(src, dst, ss, rs, e, j):
        return pltpu.make_async_remote_copy(
            src_ref=src, dst_ref=dst, send_sem=ss, recv_sem=rs, device_id=(e, j), device_id_type=MESH
        )

    loads = [
        pltpu.make_async_copy(wg_hbm.at[0], wg, w_sem.at[0]),
        pltpu.make_async_copy(wu_hbm.at[0], wu, w_sem.at[1]),
        pltpu.make_async_copy(wd_hbm.at[0], wd, w_sem.at[2]),
        pltpu.make_async_copy(wm_hbm, wm, w_sem.at[3]),
    ]
    barrier = pltpu.get_barrier_semaphore()
    for d in range(1, ep):
        pl.semaphore_signal(barrier, inc=1, device_id=(ring(me + d, ep), t), device_id_type=MESH)
    for dy in range(1, ny):
        pl.semaphore_signal(barrier, inc=1, device_id=(me, up_y(dy) * 2 + c), device_id_type=MESH)
    pl.semaphore_signal(barrier, inc=1, device_id=(me, mate), device_id_type=MESH)
    for load in loads:
        load.start()

    i_r = lax.broadcasted_iota(jnp.int32, (rows, rows), 0)
    i_c = lax.broadcasted_iota(jnp.int32, (rows, rows), 1)
    lane = lax.broadcasted_iota(jnp.int32, (rows, 128), 1)
    slot_lane = lax.broadcasted_iota(jnp.int32, (rows, slots), 1)
    rel, hot = [], []
    for k in range(TOP_K):
        e = rt_ref[:, k : k + 1]
        r = jnp.where(e >= me, e - me, e - me + ep)
        rel.append(r)
        hot.append((lane == r).astype(F32))
    before = mm((i_r > i_c).astype(F32).astype(BF), sum(hot).astype(BF))
    both = None
    for k in range(TOP_K):
        rank = jnp.sum(before * hot[k], axis=1, keepdims=True).astype(jnp.int32)
        p = (slot_lane == rel[k] * cap + rank).astype(F32)
        both = p if both is None else both + p
        pick[k] = p.astype(BF)
    xf = x_ref[...].astype(F32)
    inv = lax.rsqrt(jnp.mean(xf * xf, axis=1, keepdims=True) + EPS)
    cols = pl.ds(pl.multiple_of(t * width, width), width)
    normed = (x_ref[:, cols].astype(F32) * inv * mg_ref[:, cols]).astype(BF)
    out = mm(both.astype(BF), normed, ((0,), (0,))).astype(BF).reshape(ep, cap, width)
    disp[...] = out
    xs[t, 0] = out[0]

    pl.semaphore_wait(barrier, ep - 1 + ny)

    def a2a(d):
        return rc(disp.at[d], xs.at[t, d], a_ss.at[d], a_rs.at[d], ring(me + d, ep), t)

    for d in range(1, ep):
        a2a(d).start()

    def gat(col, g):
        return xs.at[col, pl.ds(g * gb, gb)]

    def gat_y(g, dy):
        r = gat(t, g)
        return rc(r, r, gy_ss.at[g, dy], gy_rs.at[g, dy], me, up_y(dy) * 2 + c)

    def gat_y_in(g, dy):
        r = gat(dn_y(dy) * 2 + c, g)
        return rc(r, r, gy_ss.at[g, dy], gy_rs.at[g, dy], me, mate)

    def gat_p(g, dy):
        r = gat(dn_y(dy) * 2 + c, g)
        return rc(r, r, gp_ss.at[g, dy], gp_rs.at[g, dy], me, mate)

    def gat_p_in(g, dy):
        r = gat(dn_y(dy) * 2 + 1 - c, g)
        return rc(r, r, gp_ss.at[g, dy], gp_rs.at[g, dy], me, mate)

    def relay1(g):
        for d in range(max(1, g * gb), (g + 1) * gb):
            a2a(d).wait_recv()
        for dy in range(1, ny):
            gat_y(g, dy).start()
        gat_p(g, 0).start()

    def relay2(g):
        for dy in range(1, ny):
            gat_y_in(g, dy).wait_recv()
            gat_p(g, dy).start()

    def arrived(g):
        for dy in range(ny):
            gat_p_in(g, dy).wait_recv()

    causal = i_r >= i_c
    tri = causal.astype(F32)

    def mix_all_decay():
        fl = ff_ref[...]
        fx = fi_ref[...].astype(F32)
        forget = fl + (1.0 - fl) * jax.nn.sigmoid(fx)
        return mm(tri, jnp.log(forget), precision=HIGH)

    def mix_head(h, run, s_col, s_row):
        hc = slice(h * hs, (h + 1) * hs)
        lr = run[:, hc]
        sc = s_col[:, h : h + 1]
        sr = s_row[h : h + 1, :]
        key = (1.0 - ff_ref[:, hc]) * jax.nn.sigmoid(-fi_ref[:, hc].astype(F32))
        q = q_ref[:, hc].astype(F32) * jnp.exp(lr)
        v = v_ref[:, hc]
        scores = mm(q.astype(BF), (key * jnp.exp(-lr)).astype(BF), ((1,), (1,)))
        scores = jnp.where(causal, scores * jnp.exp(jnp.minimum(sc - sr, 0.0)), 0.0)
        intra[:, hc] = mm(scores.astype(BF), v)
        qdec[:, hc] = (q * jnp.exp(sc)).astype(BF)
        l_end = lr[rows - 1 : rows, :]
        s_end = sc[rows - 1 : rows, :]
        kd = (key * jnp.exp(l_end - lr + (s_end - sc))).astype(BF)
        ks_s[0, h, 0:hs, :] = mm(v, kd, ((0,), (0,))).astype(BF)
        ks_s[0, h, hs : hs + 16, :] = jnp.broadcast_to(jnp.exp(l_end + s_end), (16, hs)).astype(BF)

    windows = scan_windows(ep)

    def scan_copy(i):
        hop = max(1, windows[i])
        return rc(ks_s.at[i], ks_r.at[i], k_ss.at[i], k_rs.at[i], ring(me + hop, ep), t)

    def scan_take(i):
        scan_copy(i).wait_recv()
        hop = max(1, windows[i])
        have = me >= hop
        for h in range(heads):
            got = ks_r[i, h].astype(F32)
            s_in = jnp.where(have, got[0:hs], 0.0)
            a_in = jnp.where(have, got[hs : hs + 16], 1.0)
            if i > 0:
                a_own = carry[h, hs : hs + 16, :]
                s_in = a_own[0:1] * s_in + carry[h, 0:hs, :]
                a_in = a_own * a_in
            carry[h, 0:hs, :] = s_in
            carry[h, hs : hs + 16, :] = a_in
            if i + 1 < len(windows):
                ks_s[i + 1, h, 0:hs, :] = s_in.astype(BF)
                ks_s[i + 1, h, hs : hs + 16, :] = a_in.astype(BF)
        if i + 1 < len(windows):
            scan_copy(i + 1).start()

    def ho_y(dy):
        return rc(ho.at[t], ho.at[t], hy_ss.at[dy], hy_rs.at[dy], me, up_y(dy) * 2 + c)

    def ho_y_in(dy):
        r = ho.at[dn_y(dy) * 2 + c]
        return rc(r, r, hy_ss.at[dy], hy_rs.at[dy], me, mate)

    def ho_p(dy):
        r = ho.at[dn_y(dy) * 2 + c]
        return rc(r, r, hp_ss.at[dy], hp_rs.at[dy], me, mate)

    def ho_p_in(dy):
        r = ho.at[dn_y(dy) * 2 + 1 - c]
        return rc(r, r, hp_ss.at[dy], hp_rs.at[dy], me, mate)

    def mix_close():
        for h in range(heads):
            hc = slice(h * hs, (h + 1) * hs)
            o = intra[:, hc] + mm(qdec[:, hc], carry[h, 0:hs, :].astype(BF), ((1,), (1,)))
            iv = lax.rsqrt(jnp.mean(o * o, axis=1, keepdims=True) + EPS)
            g = og_ref[:, hc].astype(F32)
            ho[t, :, hc] = (o * iv * hg_ref[...] * (g * jax.nn.sigmoid(g))).astype(BF)
        for dy in range(1, ny):
            ho_y(dy).start()
        ho_p(0).start()

    def ho_relay():
        for dy in range(1, ny):
            ho_y_in(dy).wait_recv()
            ho_p(dy).start()

    gr = gb * cap
    ft = min(256, hidden_units)

    def first(g):
        def tile(n, _):
            fc = pl.ds(pl.multiple_of(n * ft, ft), ft)
            gate = jnp.zeros((gr, ft), F32)
            up = jnp.zeros((gr, ft), F32)
            for j in range(tp):
                a = xs[j, g * gb : (g + 1) * gb].reshape(gr, width)
                gate += mm(a, wg[j * width : (j + 1) * width, fc])
                up += mm(a, wu[j * width : (j + 1) * width, fc])
            hid[:, fc] = (gate * jax.nn.sigmoid(gate) * up).astype(BF)
            return 0

        lax.fori_loop(0, hidden_units // ft, tile, 0)

    def down(dy, core):
        col = up_y(dy) * 2 + core
        return mm(hid[...], wd[:, pl.ds(pl.multiple_of(col * width, width), width)])

    def red_p(g, dy):
        return rc(snd_p.at[g, dy], rs_p.at[g, dy], rp_ss.at[g, dy], rp_rs.at[g, dy], me, mate)

    def red_y(g, dy):
        return rc(
            snd_y.at[g, dy], rs_y.at[g, dy], ry_ss.at[g, dy], ry_rs.at[g, dy], me, up_y(dy) * 2 + c
        )

    order = list(range(1, ny)) + [0]

    def second(g):
        for dy in order:
            snd_p[g, dy] = down(dy, 1 - c).astype(BF)
            red_p(g, dy).start()
        for dy in order:
            own[g % 2, dy] = down(dy, c)
        for dy in order:
            red_p(g, dy).wait_recv()
            total = own[g % 2, dy] + rs_p[g, dy].astype(F32)
            if dy:
                snd_y[g, dy] = total.astype(BF)
                red_y(g, dy).start()
            else:
                own[g % 2, 0] = total

    def back(d):
        return rc(fin.at[d], ret.at[d], b_ss.at[d], b_rs.at[d], ring(me - d, ep), t)

    def third(g):
        total = own[g % 2, 0]
        for dy in range(1, ny):
            red_y(g, dy).wait_recv()
            total += rs_y[g, dy].astype(F32)
        blocks = total.astype(BF).reshape(gb, cap, width)
        for i in range(gb):
            d = g * gb + i
            if d == 0:
                ret[0] = blocks[0]
            else:
                fin[d] = blocks[i]
                back(d).start()

    run = mix_all_decay()
    s_col = mm(tri, ds_ref[...], precision=HIGH)
    s_row = mm(ds_ref[...], (i_r <= i_c).astype(F32), ((0,), (0,)), precision=HIGH)
    for h in range(heads):
        mix_head(h, run, s_col, s_row)
        if h == heads // 2:
            relay1(0)
    scan_copy(0).start()
    relay1(1)
    relay2(0)
    scan_take(0)
    relay1(2)
    for load in loads[:3]:
        load.wait()
    taken = 1
    for g in range(groups):
        arrived(g)
        first(g)
        if g + 1 < groups:
            relay2(g + 1)
        if g + 3 < groups:
            relay1(g + 3)
        second(g)
        if taken < len(windows):
            scan_take(taken)
            taken += 1
        if g > 0:
            third(g - 1)
    while taken < len(windows):
        scan_take(taken)
        taken += 1
    mix_close()
    third(groups - 1)
    ho_relay()
    loads[3].wait()
    for dy in range(ny):
        ho_p_in(dy).wait_recv()
    acc = jnp.zeros(mixed_ref.shape, F32)
    for j in range(tp):
        acc += mm(ho[j], wm[j * hw : (j + 1) * hw, :])
    mixed_ref[...] = acc.astype(BF)
    for d in range(1, ep):
        back(d).wait_recv()
    flat = ret[...].reshape(slots, width)
    res = jnp.zeros(moe_ref.shape, F32)
    for k in range(TOP_K):
        res += mm(pick[k], flat) * rw_ref[:, k : k + 1]
    moe_ref[...] = res.astype(BF)

    for d in range(1, ep):
        a2a(d).wait_send()
        back(d).wait_send()
    for i in range(len(windows)):
        scan_copy(i).wait_send()
    for dy in range(ny):
        ho_p(dy).wait_send()
        if dy:
            ho_y(dy).wait_send()
        for g in range(groups):
            gat_p(g, dy).wait_send()
            red_p(g, dy).wait_send()
            if dy:
                gat_y(g, dy).wait_send()
                red_y(g, dy).wait_send()


def body(ep, tp, *args):
    (q, fi, v, og, ds, ff, hg, wm, x, mg, rt, rw, wg, wu, wd) = args
    rows, dim = x.shape
    capacity = 5 * rows * TOP_K // (4 * ep)
    cap = -(-capacity // 16) * 16
    groups = 4
    gb = ep // groups
    ny = tp // 2
    width = dim // tp
    heads = ds.shape[1]
    hs = hg.shape[0]
    hw = q.shape[1]
    steps = len(scan_windows(ep))
    fu = wg.shape[2]
    gr = gb * cap
    vm = pltpu.VMEM
    dma = pltpu.SemaphoreType.DMA
    scratch = [
        vm(wm.shape, BF),
        vm(wg.shape[1:], BF),
        vm(wu.shape[1:], BF),
        vm(wd.shape[1:], BF),
        vm((ep, cap, width), BF),
        vm((tp, ep, cap, width), BF),
        vm((gr, fu), BF),
        vm((groups, ny, gr, width), BF),
        vm((groups, ny, gr, width), BF),
        vm((2, ny, gr, width), F32),
        vm((groups, ny, gr, width), BF),
        vm((groups, ny, gr, width), BF),
        vm((ep, cap, width), BF),
        vm((ep, cap, width), BF),
        vm((TOP_K, rows, ep * cap), BF),
        vm((steps, heads, hs + 16, hs), BF),
        vm((steps, heads, hs + 16, hs), BF),
        vm((heads, hs + 16, hs), F32),
        vm((rows, hw), F32),
        vm((rows, hw), BF),
        vm((tp, rows, hw), BF),
        dma((4,)),
        dma((ep,)),
        dma((ep,)),
        dma((groups, ny)),
        dma((groups, ny)),
        dma((groups, ny)),
        dma((groups, ny)),
        dma((groups, ny)),
        dma((groups, ny)),
        dma((groups, ny)),
        dma((groups, ny)),
        dma((ep,)),
        dma((ep,)),
        dma((steps,)),
        dma((steps,)),
        dma((ny,)),
        dma((ny,)),
        dma((ny,)),
        dma((ny,)),
    ]
    out = jax.ShapeDtypeStruct((rows, width), BF)
    in_vm = pl.BlockSpec(memory_space=pltpu.VMEM)
    in_any = pl.BlockSpec(memory_space=pl.ANY)
    return pl.pallas_call(
        functools.partial(kernel, (ep, tp, cap, groups)),
        out_shape=(out, out),
        in_specs=[in_vm] * 11 + [in_any] * 4,
        out_specs=(in_vm, in_vm),
        scratch_shapes=scratch,
        compiler_params=pltpu.CompilerParams(
            collective_id=0, has_side_effects=True, vmem_limit_bytes=60 * 1024 * 1024
        ),
    )(q, fi, v, og, ds, ff[None, :], hg[None, :], x, mg[None, :], rt, rw, wm, wg, wu, wd)


def solution(mesh):
    placed = (
        P("ep", "tp"),
        P("ep", "tp"),
        P("ep", "tp"),
        P("ep", "tp"),
        P("ep", "tp"),
        P("tp"),
        P(),
        P(None, "tp"),
        P("ep", None),
        P(),
        P("ep", None),
        P("ep", None),
        P("ep", None, "tp"),
        P("ep", None, "tp"),
        P("ep", "tp", None),
    )
    return jax.shard_map(
        functools.partial(body, mesh.shape["ep"], mesh.shape["tp"]),
        mesh=mesh,
        in_specs=placed,
        out_specs=(P("ep", "tp"), P("ep", "tp")),
        check_vma=False,
    )
```

```python
import functools

import jax
import jax.numpy as jnp
from jax import lax
from jax.experimental import pallas as pl
from jax.experimental.pallas import tpu as pltpu
from jax.sharding import PartitionSpec as P

TOP_K = 2
EPS = 1e-06
MESH = pl.DeviceIdType.MESH
BF = jnp.bfloat16
F32 = jnp.float32
HIGH = lax.Precision.HIGHEST


def mm(a, b, dims=((1,), (0,)), precision=None):
    return lax.dot_general(
        a, b, (dims, ((), ())), preferred_element_type=F32, precision=precision
    )


def scan_windows(ep):
    windows = [0]
    w = 1
    while w < ep - 1:
        windows.append(w)
        w *= 2
    return windows


def kernel(
    cfg,
    q_ref,
    fi_ref,
    v_ref,
    og_ref,
    ds_ref,
    ff_ref,
    hg_ref,
    x_ref,
    mg_ref,
    rt_ref,
    rw_ref,
    wm_hbm,
    wg_hbm,
    wu_hbm,
    wd_hbm,
    mixed_ref,
    moe_ref,
    wm,
    wg,
    wu,
    wd,
    disp,
    xs,
    hid,
    snd_p,
    rs_p,
    own,
    snd_y,
    rs_y,
    fin,
    ret,
    pick,
    ks_s,
    ks_r,
    carry,
    intra,
    qdec,
    ho,
    w_sem,
    a_ss,
    a_rs,
    gy_ss,
    gy_rs,
    gp_ss,
    gp_rs,
    rp_ss,
    rp_rs,
    ry_ss,
    ry_rs,
    b_ss,
    b_rs,
    k_ss,
    k_rs,
    hy_ss,
    hy_rs,
    hp_ss,
    hp_rs,
):
    ep, tp, cap, groups = cfg
    gb = ep // groups
    ny = tp // 2
    me = lax.axis_index("ep")
    t = lax.axis_index("tp")
    y = t // 2
    c = t % 2
    mate = y * 2 + (1 - c)
    rows, dim = x_ref.shape
    width = dim // tp
    slots = ep * cap
    hidden_units = wg.shape[1]
    heads = ds_ref.shape[0]
    hs = hg_ref.shape[1]
    hw = q_ref.shape[1]

    def ring(a, n):
        return lax.rem(a + n, n)

    def up_y(dy):
        return ring(y + dy, ny)

    def dn_y(dy):
        return ring(y - dy, ny)

    def rc(src, dst, ss, rs, e, j):
        return pltpu.make_async_remote_copy(
            src_ref=src, dst_ref=dst, send_sem=ss, recv_sem=rs, device_id=(e, j), device_id_type=MESH
        )

    loads = [
        pltpu.make_async_copy(wg_hbm.at[0], wg, w_sem.at[0]),
        pltpu.make_async_copy(wu_hbm.at[0], wu, w_sem.at[1]),
        pltpu.make_async_copy(wd_hbm.at[0], wd, w_sem.at[2]),
        pltpu.make_async_copy(wm_hbm, wm, w_sem.at[3]),
    ]
    barrier = pltpu.get_barrier_semaphore()
    for d in range(1, ep):
        pl.semaphore_signal(barrier, inc=1, device_id=(ring(me + d, ep), t), device_id_type=MESH)
    for dy in range(1, ny):
        pl.semaphore_signal(barrier, inc=1, device_id=(me, up_y(dy) * 2 + c), device_id_type=MESH)
    pl.semaphore_signal(barrier, inc=1, device_id=(me, mate), device_id_type=MESH)
    for load in loads:
        load.start()

    i_r = lax.broadcasted_iota(jnp.int32, (rows, rows), 0)
    i_c = lax.broadcasted_iota(jnp.int32, (rows, rows), 1)
    lane = lax.broadcasted_iota(jnp.int32, (rows, 128), 1)
    slot_lane = lax.broadcasted_iota(jnp.int32, (rows, slots), 1)
    eye = (i_r == i_c).astype(F32)
    ids = mm(eye, rt_ref[...].astype(F32), ((1,), (1,)), HIGH).astype(jnp.int32)
    rel, hot = [], []
    for k in range(TOP_K):
        e = ids[:, k : k + 1]
        r = jnp.where(e >= me, e - me, e - me + ep)
        rel.append(r)
        hot.append((lane == r).astype(F32))
    before = mm((i_r > i_c).astype(F32).astype(BF), sum(hot).astype(BF))
    both = None
    for k in range(TOP_K):
        rank = jnp.sum(before * hot[k], axis=1, keepdims=True).astype(jnp.int32)
        p = (slot_lane == rel[k] * cap + rank).astype(F32)
        both = p if both is None else both + p
        pick[k] = p.astype(BF)
    xf = x_ref[...].astype(F32)
    inv = lax.rsqrt(jnp.mean(xf * xf, axis=1, keepdims=True) + EPS)
    cols = pl.ds(pl.multiple_of(t * width, width), width)
    normed = (x_ref[:, cols].astype(F32) * inv * mg_ref[:, cols]).astype(BF)
    out = mm(both.astype(BF), normed, ((0,), (0,))).astype(BF).reshape(ep, cap, width)
    disp[...] = out
    xs[t, 0] = out[0]

    pl.semaphore_wait(barrier, ep - 1 + ny)

    def a2a(d):
        return rc(disp.at[d], xs.at[t, d], a_ss.at[d], a_rs.at[d], ring(me + d, ep), t)

    for d in range(1, ep):
        a2a(d).start()

    def gat(col, g):
        return xs.at[col, pl.ds(g * gb, gb)]

    def gat_y(g, dy):
        r = gat(t, g)
        return rc(r, r, gy_ss.at[g, dy], gy_rs.at[g, dy], me, up_y(dy) * 2 + c)

    def gat_y_in(g, dy):
        r = gat(dn_y(dy) * 2 + c, g)
        return rc(r, r, gy_ss.at[g, dy], gy_rs.at[g, dy], me, mate)

    def gat_p(g, dy):
        r = gat(dn_y(dy) * 2 + c, g)
        return rc(r, r, gp_ss.at[g, dy], gp_rs.at[g, dy], me, mate)

    def gat_p_in(g, dy):
        r = gat(dn_y(dy) * 2 + 1 - c, g)
        return rc(r, r, gp_ss.at[g, dy], gp_rs.at[g, dy], me, mate)

    def relay1(g):
        for d in range(max(1, g * gb), (g + 1) * gb):
            a2a(d).wait_recv()
        for dy in range(1, ny):
            gat_y(g, dy).start()
        gat_p(g, 0).start()

    def relay2(g):
        for dy in range(1, ny):
            gat_y_in(g, dy).wait_recv()
            gat_p(g, dy).start()

    def arrived(g):
        for dy in range(ny):
            gat_p_in(g, dy).wait_recv()

    causal = i_r >= i_c
    tri = causal.astype(F32)

    def mix_all_decay():
        fl = ff_ref[...]
        fx = fi_ref[...].astype(F32)
        forget = fl + (1.0 - fl) * jax.nn.sigmoid(fx)
        return mm(tri, jnp.log(forget), precision=HIGH)

    def mix_head(h, run, s_col, s_row):
        hc = slice(h * hs, (h + 1) * hs)
        lr = run[:, hc]
        sc = s_col[:, h : h + 1]
        sr = s_row[h : h + 1, :]
        key = (1.0 - ff_ref[:, hc]) * jax.nn.sigmoid(-fi_ref[:, hc].astype(F32))
        q = q_ref[:, hc].astype(F32) * jnp.exp(lr)
        v = v_ref[:, hc]
        scores = mm(q.astype(BF), (key * jnp.exp(-lr)).astype(BF), ((1,), (1,)))
        scores = jnp.where(causal, scores * jnp.exp(jnp.minimum(sc - sr, 0.0)), 0.0)
        intra[:, hc] = mm(scores.astype(BF), v)
        qdec[:, hc] = (q * jnp.exp(sc)).astype(BF)
        l_end = lr[rows - 1 : rows, :]
        s_end = sc[rows - 1 : rows, :]
        kd = (key * jnp.exp(l_end - lr + (s_end - sc))).astype(BF)
        ks_s[0, h, 0:hs, :] = mm(v, kd, ((0,), (0,))).astype(BF)
        ks_s[0, h, hs : hs + 16, :] = jnp.broadcast_to(jnp.exp(l_end + s_end), (16, hs)).astype(BF)

    windows = scan_windows(ep)

    def scan_copy(i):
        hop = max(1, windows[i])
        return rc(ks_s.at[i], ks_r.at[i], k_ss.at[i], k_rs.at[i], ring(me + hop, ep), t)

    def scan_send(i, act):
        pl.when(me + max(1, windows[i]) < ep)(lambda: act(scan_copy(i)))

    def scan_take(i):
        hop = max(1, windows[i])
        have = me >= hop

        @pl.when(jnp.logical_not(have))
        def _():
            ks_r[i] = jnp.zeros(ks_r.shape[1:], BF)

        pl.when(have)(lambda: scan_copy(i).wait_recv())
        for h in range(heads):
            got = ks_r[i, h].astype(F32)
            s_in = jnp.where(have, got[0:hs], 0.0)
            a_in = jnp.where(have, got[hs : hs + 16], 1.0)
            if i > 0:
                a_own = carry[h, hs : hs + 16, :]
                s_in = a_own[0:1] * s_in + carry[h, 0:hs, :]
                a_in = a_own * a_in
            carry[h, 0:hs, :] = s_in
            carry[h, hs : hs + 16, :] = a_in
            if i + 1 < len(windows):
                ks_s[i + 1, h, 0:hs, :] = s_in.astype(BF)
                ks_s[i + 1, h, hs : hs + 16, :] = a_in.astype(BF)
        if i + 1 < len(windows):
            scan_send(i + 1, lambda a: a.start())

    def ho_y(dy):
        return rc(ho.at[t], ho.at[t], hy_ss.at[dy], hy_rs.at[dy], me, up_y(dy) * 2 + c)

    def ho_y_in(dy):
        r = ho.at[dn_y(dy) * 2 + c]
        return rc(r, r, hy_ss.at[dy], hy_rs.at[dy], me, mate)

    def ho_p(dy):
        r = ho.at[dn_y(dy) * 2 + c]
        return rc(r, r, hp_ss.at[dy], hp_rs.at[dy], me, mate)

    def ho_p_in(dy):
        r = ho.at[dn_y(dy) * 2 + 1 - c]
        return rc(r, r, hp_ss.at[dy], hp_rs.at[dy], me, mate)

    def mix_close():
        for h in range(heads):
            hc = slice(h * hs, (h + 1) * hs)
            o = intra[:, hc] + mm(qdec[:, hc], carry[h, 0:hs, :].astype(BF), ((1,), (1,)))
            iv = lax.rsqrt(jnp.mean(o * o, axis=1, keepdims=True) + EPS)
            g = og_ref[:, hc].astype(F32)
            ho[t, :, hc] = (o * iv * hg_ref[...] * (g * jax.nn.sigmoid(g))).astype(BF)
        for dy in range(1, ny):
            ho_y(dy).start()
        ho_p(0).start()

    def ho_relay():
        for dy in range(1, ny):
            ho_y_in(dy).wait_recv()
            ho_p(dy).start()

    gr = gb * cap
    ft = min(256, hidden_units)

    def first(g):
        def tile(n, _):
            fc = pl.ds(pl.multiple_of(n * ft, ft), ft)
            gate = jnp.zeros((gr, ft), F32)
            up = jnp.zeros((gr, ft), F32)
            for j in range(tp):
                a = xs[j, g * gb : (g + 1) * gb].reshape(gr, width)
                gate += mm(a, wg[j * width : (j + 1) * width, fc])
                up += mm(a, wu[j * width : (j + 1) * width, fc])
            hid[:, fc] = (gate * jax.nn.sigmoid(gate) * up).astype(BF)
            return 0

        lax.fori_loop(0, hidden_units // ft, tile, 0)

    def down(dy, core):
        col = up_y(dy) * 2 + core
        return mm(hid[...], wd[:, pl.ds(pl.multiple_of(col * width, width), width)])

    def red_p(g, dy):
        return rc(snd_p.at[g, dy], rs_p.at[g, dy], rp_ss.at[g, dy], rp_rs.at[g, dy], me, mate)

    def red_y(g, dy):
        return rc(
            snd_y.at[g, dy], rs_y.at[g, dy], ry_ss.at[g, dy], ry_rs.at[g, dy], me, up_y(dy) * 2 + c
        )

    order = list(range(1, ny)) + [0]

    def second(g):
        for dy in order:
            snd_p[g, dy] = down(dy, 1 - c).astype(BF)
            red_p(g, dy).start()
        for dy in order:
            own[g % 2, dy] = down(dy, c)
        for dy in order:
            red_p(g, dy).wait_recv()
            total = own[g % 2, dy] + rs_p[g, dy].astype(F32)
            if dy:
                snd_y[g, dy] = total.astype(BF)
                red_y(g, dy).start()
            else:
                own[g % 2, 0] = total

    def back(d):
        return rc(fin.at[d], ret.at[d], b_ss.at[d], b_rs.at[d], ring(me - d, ep), t)

    def third(g):
        total = own[g % 2, 0]
        for dy in range(1, ny):
            red_y(g, dy).wait_recv()
            total += rs_y[g, dy].astype(F32)
        blocks = total.astype(BF).reshape(gb, cap, width)
        for i in range(gb):
            d = g * gb + i
            if d == 0:
                ret[0] = blocks[0]
            else:
                fin[d] = blocks[i]
                back(d).start()

    run = mix_all_decay()
    s_col = mm(tri, ds_ref[...], ((1,), (1,)), HIGH)
    s_row = mm(ds_ref[...], tri, ((1,), (1,)), HIGH)
    for h in range(heads):
        mix_head(h, run, s_col, s_row)
        if h == heads // 2:
            relay1(0)
    scan_send(0, lambda a: a.start())
    relay1(1)
    relay2(0)
    scan_take(0)
    relay1(2)
    for load in loads[:3]:
        load.wait()
    taken = 1
    for g in range(groups):
        arrived(g)
        first(g)
        if g + 1 < groups:
            relay2(g + 1)
        if g + 3 < groups:
            relay1(g + 3)
        second(g)
        if taken < len(windows):
            scan_take(taken)
            taken += 1
        if g > 0:
            third(g - 1)
    while taken < len(windows):
        scan_take(taken)
        taken += 1
    mix_close()
    third(groups - 1)
    ho_relay()
    loads[3].wait()
    for dy in range(ny):
        ho_p_in(dy).wait_recv()
    acc = jnp.zeros(mixed_ref.shape, F32)
    for j in range(tp):
        acc += mm(ho[j], wm[j * hw : (j + 1) * hw, :])
    mixed_ref[...] = acc.astype(BF)
    for d in range(1, ep):
        back(d).wait_recv()
    flat = ret[...].reshape(slots, width)
    res = jnp.zeros(moe_ref.shape, F32)
    weight = mm(eye, rw_ref[...], ((1,), (1,)), HIGH)
    for k in range(TOP_K):
        res += mm(pick[k], flat) * weight[:, k : k + 1]
    moe_ref[...] = res.astype(BF)

    for d in range(1, ep):
        a2a(d).wait_send()
        back(d).wait_send()
    for i in range(len(windows)):
        scan_send(i, lambda a: a.wait_send())
    for dy in range(ny):
        ho_p(dy).wait_send()
        if dy:
            ho_y(dy).wait_send()
        for g in range(groups):
            gat_p(g, dy).wait_send()
            red_p(g, dy).wait_send()
            if dy:
                gat_y(g, dy).wait_send()
                red_y(g, dy).wait_send()


def emit(a_ref, b_ref, a_out, b_out):
    a_out[...] = a_ref[...]
    b_out[...] = b_ref[...]


def body(ep, tp, *args):
    (q, fi, v, og, ds, ff, hg, wm, x, mg, rt, rw, wg, wu, wd) = args
    rows, dim = x.shape
    capacity = 5 * rows * TOP_K // (4 * ep)
    cap = -(-capacity // 16) * 16
    groups = 4
    gb = ep // groups
    ny = tp // 2
    width = dim // tp
    heads = ds.shape[1]
    hs = hg.shape[0]
    hw = q.shape[1]
    steps = len(scan_windows(ep))
    fu = wg.shape[2]
    gr = gb * cap
    vm = pltpu.VMEM
    dma = pltpu.SemaphoreType.DMA
    scratch = [
        vm(wm.shape, BF),
        vm(wg.shape[1:], BF),
        vm(wu.shape[1:], BF),
        vm(wd.shape[1:], BF),
        vm((ep, cap, width), BF),
        vm((tp, ep, cap, width), BF),
        vm((gr, fu), BF),
        vm((groups, ny, gr, width), BF),
        vm((groups, ny, gr, width), BF),
        vm((2, ny, gr, width), F32),
        vm((groups, ny, gr, width), BF),
        vm((groups, ny, gr, width), BF),
        vm((ep, cap, width), BF),
        vm((ep, cap, width), BF),
        vm((TOP_K, rows, ep * cap), BF),
        vm((steps, heads, hs + 16, hs), BF),
        vm((steps, heads, hs + 16, hs), BF),
        vm((heads, hs + 16, hs), F32),
        vm((rows, hw), F32),
        vm((rows, hw), BF),
        vm((tp, rows, hw), BF),
        dma((4,)),
        dma((ep,)),
        dma((ep,)),
        dma((groups, ny)),
        dma((groups, ny)),
        dma((groups, ny)),
        dma((groups, ny)),
        dma((groups, ny)),
        dma((groups, ny)),
        dma((groups, ny)),
        dma((groups, ny)),
        dma((ep,)),
        dma((ep,)),
        dma((steps,)),
        dma((steps,)),
        dma((ny,)),
        dma((ny,)),
        dma((ny,)),
        dma((ny,)),
    ]
    out = jax.ShapeDtypeStruct((rows, width), BF)
    in_vm = pl.BlockSpec(memory_space=pltpu.VMEM)
    in_any = pl.BlockSpec(memory_space=pl.ANY)
    made = pl.pallas_call(
        functools.partial(kernel, (ep, tp, cap, groups)),
        out_shape=(out, out),
        in_specs=[in_vm] * 11 + [in_any] * 4,
        out_specs=(in_vm, in_vm),
        scratch_shapes=scratch,
        compiler_params=pltpu.CompilerParams(
            collective_id=0, has_side_effects=True, vmem_limit_bytes=60 * 1024 * 1024
        ),
    )(q, fi, v, og, ds.T, ff[None, :], hg[None, :], x, mg[None, :], rt.T, rw.T, wm, wg, wu, wd)
    return pl.pallas_call(
        emit, out_shape=(out, out), in_specs=[in_vm] * 2, out_specs=(in_vm, in_vm), name="emit"
    )(*made)


def solution(mesh):
    placed = (
        P("ep", "tp"),
        P("ep", "tp"),
        P("ep", "tp"),
        P("ep", "tp"),
        P("ep", "tp"),
        P("tp"),
        P(),
        P(None, "tp"),
        P("ep", None),
        P(),
        P("ep", None),
        P("ep", None),
        P("ep", None, "tp"),
        P("ep", None, "tp"),
        P("ep", "tp", None),
    )
    return jax.shard_map(
        functools.partial(body, mesh.shape["ep"], mesh.shape["tp"]),
        mesh=mesh,
        in_specs=placed,
        out_specs=(P("ep", "tp"), P("ep", "tp")),
        check_vma=False,
    )
```
